32 devices in a mesh: sp: 8 (over z, core), tp: 4 (over y, x).
Axes of the slice: x: 2, y: 2, z: 4, core: 2. Of those that a mesh axis runs over, the one named last changes fastest.
Arguments:
- mix_values: bfloat16 [1024, 4096], P('sp', 'tp'), may hold values from -6 to 6
- mix_gate: bfloat16 [1024, 4096], P('sp', 'tp'), may hold values from -6 to 6
- input_keys: bfloat16 [1024, 2048], P('sp', 'tp'), may hold values from -0.31640625 to 0.31640625
- output_keys: bfloat16 [1024, 2048], P('sp', 'tp'), may hold values from -0.31640625 to 0.31640625
- step_sizes: float32 [1024, 64], P('sp', 'tp'), may hold values from 0.1 to 8
- decay_rates: float32 [64], P('tp'), may hold values from 4.8828125e-05 to 0.03
- out_proj: bfloat16 [2048, 4096], P('sp', 'tp'), may hold values from -0.09375 to 0.09375
- expert_inputs: bfloat16 [1024, 2048], P('sp'), may hold values from -20 to 20
- stream_grad: bfloat16 [1024, 2048], P('sp'), may hold values from -6 to 6
- routes: int32 [1024, 2], P('sp'), may hold values from 0 to 7, all different within a row; in each aligned block of 128 rows (0 to 127, 128 to 255, ...) at most 48 rows name the same one
- route_weights: float32 [1024, 2], P('sp'), may hold values from 0.1 to 0.9
- gate_proj: bfloat16 [8, 2048, 2048], P('sp', 'tp'), may hold values from -0.125 to 0.125
- up_proj: bfloat16 [8, 2048, 2048], P('sp', 'tp'), may hold values from -0.125 to 0.125
- down_proj: bfloat16 [8, 2048, 2048], P('sp', 'tp'), may hold values from -0.125 to 0.125
Outputs:
- grad_gate_proj: bfloat16 [8, 2048, 2048], P('sp', 'tp')
- grad_up_proj: bfloat16 [8, 2048, 2048], P('sp', 'tp')
- grad_down_proj: bfloat16 [8, 2048, 2048], P('sp', 'tp')
- grad_out_proj: float32 [2048, 4096], P('sp', 'tp')
- grad_values: bfloat16 [1024, 4096], P('sp', 'tp')
- grad_gate: bfloat16 [1024, 4096], P('sp', 'tp')
- grad_input_keys: bfloat16 [1024, 2048], P('sp', 'tp')
- grad_output_keys: bfloat16 [1024, 2048], P('sp', 'tp')
- grad_steps: float32 [1024, 64], P('sp', 'tp')
The draws below stay inside these ranges and needn't reach their ends.
Inputs may be any that keep to these rules, and one draw needn't show every extreme that they name: In the rows of one device no expert is named by more than 48 routes, and on some devices one expert is named by exactly 48; the 2 routes of a token name different experts.
All inputs are finite; a program needn't handle non-finite values.
Results may differ from the reference program's by a relative error of at most 0.025.
Values may be sent and summed in bfloat16 or wider, within the bound.
A program may use at most 64 MiB of HBM per device.

```python
import math
import jax
import jax.numpy as jnp
import numpy as np
from jax import lax

D = 2048
HEAD_DIM = 64
HEADS = 64
GROUPS = 16
NSTATE = 128
BLOCK = 128
F = 2048
TOPK = 2
TOK_DEV = 128
DI = 4096
EXPERTS = 8
TOKENS = 1024
CAP = 48
N_SP = 8


def draw_decay_rates(key, part):
    choose_key, fast_key, slow_key = jax.random.split(jax.random.fold_in(key, 11), 3)
    share = 0.5
    fast_heads = jax.random.uniform(choose_key, (HEADS,), jnp.float32) < share
    fast_rate = jnp.exp(jax.random.uniform(fast_key, (HEADS,), jnp.float32, jnp.log(0.01), jnp.log(0.03)))
    slow_rate = jnp.exp(jax.random.uniform(slow_key, (HEADS,), jnp.float32, jnp.log(0.05), jnp.log(0.5))) / TOKENS
    return jnp.where(fast_heads, fast_rate, slow_rate).astype(jnp.float32)


def draw_step_sizes(key, part):
    base_key, block_key = jax.random.split(jax.random.fold_in(key, 23), 2)
    base = jnp.exp(jax.random.uniform(base_key, (TOKENS, HEADS), jnp.float32, -0.7, 0.7))
    factor = jnp.exp(jax.random.uniform(block_key, (TOKENS // BLOCK, 1), jnp.float32, jnp.log(0.4), jnp.log(2.5)))
    return (base * jnp.repeat(factor, BLOCK, axis=0)).astype(jnp.float32)


def draw_expert_inputs(key, part):
    base_key, pick_key, scale_key = jax.random.split(jax.random.fold_in(key, 37), 3)
    base = jnp.clip(jax.random.normal(base_key, (TOKENS, D), jnp.float32), -2.5, 2.5)
    picked = jax.random.uniform(pick_key, (TOKENS, 1), jnp.float32) < 0.0625
    row_scale = jax.random.uniform(scale_key, (TOKENS, 1), jnp.float32, 5.0, 8.0)
    return (base * jnp.where(picked, row_scale, 1.0)).astype(jnp.bfloat16)


def with_spikes(array, key, source, target, parts, factor):
    owner, partner = [(jnp.arange(array.shape[axis_at]) // (array.shape[axis_at] // parts)).reshape([-1 if axis == axis_at else 1 for axis in range(array.ndim)]) for axis_at in (source, target)]
    chosen = jax.random.permutation(key, parts)[partner]
    strong = (owner == chosen) | (owner == (partner + parts // 2) % parts)
    return jnp.where(strong, factor * array, array)


def levels(stream_key, dims, cuts, low, top_value):
    def one(position, parts):
        heights = jax.random.uniform(jax.random.fold_in(jax.random.fold_in(stream_key, 6), position), (parts,), jnp.float32, low / len(cuts), top_value / len(cuts))
        return jnp.repeat(jnp.exp(heights), dims[position] // parts).reshape((-1,) + (1,) * (len(dims) - position - 1))

    loudness = one(*cuts[0])
    for cut in cuts[1:]:
        loudness = loudness * one(*cut)
    return loudness


def assign_block(rng, own, number, rows, number_of, top, bound, skew):
    sequence = jax.random.permutation(rng, number_of)
    crowded, usual = shares(number_of, rows * top, bound, skew, True), shares(number_of, rows * top, bound, skew, False)
    places = jnp.arange(number_of)

    def named(lengths, turn):
        used = int((lengths > 0).sum())
        fixed = max(1, used // 4)
        moved = fixed + (places - fixed + turn * (used - fixed)) % max(1, number_of - fixed)
        return jnp.zeros((number_of,), jnp.int32).at[sequence[jnp.where(places < fixed, places, moved)]].set(jnp.asarray(lengths, jnp.int32))

    lengths = jnp.where(number % 4 == 0, named(crowded, number // 4), named(usual, number - number // 4 - 1))
    mixed = jax.random.permutation(jax.random.fold_in(own, 3), number_of)
    donor, receiver = mixed[0:number_of // 2 * 2:2], mixed[1:number_of // 2 * 2:2]
    room = jnp.minimum(lengths[donor] - 1, bound - lengths[receiver]) // 2
    room = jnp.where((donor == sequence[0]) | (receiver == sequence[0]) | (lengths[receiver] == 0), 0, jnp.maximum(room, 0))
    moved = jax.random.randint(jax.random.fold_in(own, 4), (number_of // 2,), 0, 1 << 20) % (room + 1)
    lengths = lengths.at[donor].add(-moved).at[receiver].add(moved)
    members = jnp.searchsorted(jnp.cumsum(lengths), jnp.arange(rows * top), side="right").astype(jnp.int32)
    table = members.reshape(top, rows).T
    table = table[jax.random.permutation(jax.random.fold_in(own, 1), rows)]
    turn = jax.random.randint(jax.random.fold_in(own, 2), (rows, 1), 0, top)
    return jnp.take_along_axis(table, (jnp.arange(top)[None, :] + turn) % top, axis=1)


def shares(count, total, most, lean, full):
    weights = [(1 << 20) // math.isqrt(standing ** lean) + 1 for standing in range(1, count + 1)]
    largest = most if full else min(most, max(-(-total // count), total * weights[0] // sum(weights)))
    least = 1 if total - largest >= count - 1 else 0
    given, spare = [largest] + [least] * (count - 1), total - largest - least * (count - 1)
    while spare > 0:
        free = [i for i in range(1, count) if given[i] < largest] or [i for i in range(1, count) if given[i] < most]
        pool, budget = sum([weights[i] for i in free]), spare
        for i in free:
            addition = min(most - given[i], max(1, budget * weights[i] // pool), spare)
            given[i] = given[i] + addition
            spare = spare - addition
    return np.array(given)


def gaussian(stream_key, dims, width, limit, shards=(), held_as=jnp.bfloat16):
    factor_of = levels(stream_key, dims, shards, -0.22, 0.18) if shards else 1.0
    result = jax.random.normal(stream_key, dims, jnp.float32) * width * factor_of
    return jnp.minimum(jnp.maximum(result, -limit), limit).astype(held_as)


def heavy_noise(own_key, shape, width, most, cuts, heavy, kind=jnp.bfloat16):
    array = width * jax.random.normal(own_key, shape, jnp.float32)
    if cuts:
        array = array * levels(own_key, shape, cuts, -0.22, 0.18)
    return jnp.clip(with_spikes(array, jax.random.fold_in(own_key, 3), *heavy), -most, most).astype(kind)


def setup_inputs(seed: int = 0) -> dict:
    key_of = jax.random.split(jax.random.key(seed), 15)
    mix_values = gaussian(key_of[0], (TOKENS, DI), 1.0, 6.0, ((0, 8), (1, 4)))
    mix_gate = gaussian(key_of[1], (TOKENS, DI), 1.0, 6.0, ((0, 8), (1, 4)))
    input_keys = gaussian(key_of[2], (TOKENS, GROUPS * NSTATE), (0.3 * TOKENS ** -0.25), 0.31640625, ((0, 8), (1, 4)))
    output_keys = gaussian(key_of[3], (TOKENS, GROUPS * NSTATE), (0.3 * TOKENS ** -0.25), 0.31640625, ((0, 8), (1, 4)))
    step_sizes = draw_step_sizes(jax.random.fold_in(key_of[14], 71), 0)
    decay_rates = draw_decay_rates(jax.random.fold_in(key_of[14], 71), 0)
    out_proj = gaussian(key_of[6], (D, DI), DI ** -0.5, 0.09375, ((0, 8), (1, 4)))
    expert_inputs = draw_expert_inputs(jax.random.fold_in(key_of[14], 71), 0)
    stream_grad = heavy_noise(key_of[8], (TOKENS, D), 1.0, 6.0, ((0, 8),), (0, 1, 8, 2.0))
    routes_keys = jax.random.split(jax.random.fold_in(key_of[9], 1), TOKENS // TOK_DEV)
    routes_turns = jax.random.permutation(jax.random.fold_in(key_of[9], 3), TOKENS // TOK_DEV)
    routes = jax.vmap(lambda own, number: assign_block(jax.random.fold_in(key_of[9], 2), own, number, TOK_DEV, EXPERTS, TOPK, CAP, 1))(routes_keys, routes_turns).reshape((TOKENS, TOPK))
    route_weights = jnp.clip(0.1 + 0.79999997 * jax.random.uniform(key_of[10], (TOKENS, TOPK), jnp.float32) ** levels(key_of[10], (TOKENS, TOPK), ((0, 8),), -0.2, 0.2), 0.1, 0.9)
    gate_proj = gaussian(key_of[11], (EXPERTS, F, D), D ** -0.5, 0.125, ((0, 8), (1, 4)))
    up_proj = gaussian(key_of[12], (EXPERTS, F, D), D ** -0.5, 0.125, ((0, 8), (1, 4)))
    down_proj = gaussian(key_of[13], (EXPERTS, F, D), F ** -0.5, 0.125, ((0, 8), (1, 4)))
    return dict(mix_values=mix_values, mix_gate=mix_gate, input_keys=input_keys, output_keys=output_keys, step_sizes=step_sizes, decay_rates=decay_rates, out_proj=out_proj, expert_inputs=expert_inputs, stream_grad=stream_grad, routes=routes, route_weights=route_weights, gate_proj=gate_proj, up_proj=up_proj, down_proj=down_proj)


CLAMP_LIMIT = 7.0
SIGMOID_SCALE = 1.702
HIGHEST = lax.Precision.HIGHEST

def decay_span(head_values, in_keys, out_keys, head_steps, head_rates, start_state):
    length = head_values.shape[0]
    num_blocks = length // BLOCK
    causal_mask = jnp.tril(jnp.ones((BLOCK, BLOCK), dtype=bool))

    def advance(carry_state, block_data):
        block_values, block_in, block_out, block_steps = block_data
        log_decay = jnp.cumsum(-block_steps * head_rates, axis=0)
        weighted = block_values * block_steps[..., None]
        ordered = jnp.transpose(log_decay, (1, 2, 0))
        log_gaps = ordered[..., :, None] - ordered[..., None, :]
        mixing = jnp.where(causal_mask, jnp.exp(jnp.where(causal_mask, log_gaps, 0.0)), 0.0)
        scores = jnp.einsum('lgn,sgn->gls', block_out, block_in, precision=HIGHEST)
        within = jnp.einsum('grls,sgrp->lgrp', scores[:, None] * mixing, weighted, precision=HIGHEST)
        carried = jnp.einsum('lgn,grpn->lgrp', block_out, carry_state, precision=HIGHEST) * jnp.exp(log_decay)[..., None]
        to_end = jnp.exp(log_decay[-1] - log_decay)
        new_state = carry_state * jnp.exp(log_decay[-1])[..., None, None] + jnp.einsum('lgn,lgrp->grpn', block_in, weighted * to_end[..., None], precision=HIGHEST)
        return (new_state, within + carried)
    blocks = tuple((whole_array.reshape((num_blocks, BLOCK) + whole_array.shape[1:]) for whole_array in (head_values, in_keys, out_keys, head_steps)))
    last_state, block_outputs = lax.scan(advance, start_state, blocks)
    return (block_outputs.reshape(head_values.shape), last_state)

def expert_backward(in_rows, grad_rows, gate_weight, up_weight, down_weight):
    contract = (((1,), (1,)), ((), ()))
    across = (((0,), (0,)), ((), ()))
    gate_pre = lax.dot_general(in_rows, gate_weight, contract, preferred_element_type=jnp.float32)
    up_pre = lax.dot_general(in_rows, up_weight, contract, preferred_element_type=jnp.float32)
    gate_clamped = jnp.minimum(gate_pre, CLAMP_LIMIT)
    up_clamped = jnp.clip(up_pre, -CLAMP_LIMIT, CLAMP_LIMIT)
    gate_sigmoid = jax.nn.sigmoid(SIGMOID_SCALE * gate_clamped)
    activation = ((up_clamped + 1.0) * gate_clamped * gate_sigmoid).astype(jnp.bfloat16)
    act_grad = lax.dot_general(grad_rows, down_weight, contract, preferred_element_type=jnp.float32)
    gate_grad = jnp.where(gate_pre < CLAMP_LIMIT, act_grad * (up_clamped + 1.0) * gate_sigmoid * (1.0 + SIGMOID_SCALE * gate_clamped * (1.0 - gate_sigmoid)), 0.0).astype(jnp.bfloat16)
    up_grad = jnp.where(jnp.abs(up_pre) < CLAMP_LIMIT, act_grad * gate_clamped * gate_sigmoid, 0.0).astype(jnp.bfloat16)
    grad_down = lax.dot_general(activation, grad_rows, across, preferred_element_type=jnp.float32).astype(jnp.bfloat16)
    grad_gate_w = lax.dot_general(gate_grad, in_rows, across, preferred_element_type=jnp.float32).astype(jnp.bfloat16)
    grad_up_w = lax.dot_general(up_grad, in_rows, across, preferred_element_type=jnp.float32).astype(jnp.bfloat16)
    input_grad = jnp.dot(gate_grad, gate_weight, preferred_element_type=jnp.float32) + jnp.dot(up_grad, up_weight, preferred_element_type=jnp.float32)
    return (grad_gate_w, grad_up_w, grad_down, input_grad)

def reference(mix_values, mix_gate, input_keys, output_keys, step_sizes, decay_rates, out_proj, expert_inputs, stream_grad, routes, route_weights, gate_proj, up_proj, down_proj):
    per_group = HEADS // GROUPS
    head_values = mix_values.astype(jnp.float32).reshape(TOKENS, GROUPS, per_group, HEAD_DIM)
    in_keys = input_keys.astype(jnp.float32).reshape(TOKENS, GROUPS, NSTATE)
    out_keys = output_keys.astype(jnp.float32).reshape(TOKENS, GROUPS, NSTATE)
    head_steps = step_sizes.reshape(TOKENS, GROUPS, per_group)
    head_rates = decay_rates.reshape(GROUPS, per_group)
    start_state = jnp.zeros((GROUPS, per_group, HEAD_DIM, NSTATE), jnp.float32)

    def mixer_only(values_in, keys_in, keys_out, steps_in):
        return decay_span(values_in, keys_in, keys_out, steps_in, head_rates, start_state)[0]
    mixer_out, back_mixer = jax.vjp(mixer_only, head_values, in_keys, out_keys, head_steps)
    gate_in = mix_gate.astype(jnp.float32).reshape(TOKENS, GROUPS, per_group, HEAD_DIM)
    gate_sigmoid = jax.nn.sigmoid(gate_in)
    gate_silu = gate_in * gate_sigmoid
    gated_out = (mixer_out * gate_silu).reshape(TOKENS, DI).astype(jnp.bfloat16)
    flat_routes = routes.reshape(-1)
    one_hot = (flat_routes[:, None] == jnp.arange(EXPERTS, dtype=jnp.int32)[None, :]).astype(jnp.int32)
    slot_rank = lax.optimization_barrier(jnp.sum((jnp.cumsum(one_hot, axis=0) - 1) * one_hot, axis=1))
    expert_slots = N_SP * CAP
    slot_index = (flat_routes * expert_slots + slot_rank).astype(jnp.int32)
    slot_table = jnp.zeros((EXPERTS * expert_slots,), jnp.int32).at[slot_index].set(jnp.arange(TOKENS * TOPK, dtype=jnp.int32) + 1)
    flat_weights = route_weights.reshape(-1)

    def expert_pass(packed):
        slot_routes, gate_weight, up_weight, down_weight = packed
        slot_used = slot_routes > 0
        route_id = jnp.maximum(slot_routes - 1, 0)
        token_id = route_id // TOPK
        route_scale = jnp.where(slot_used, flat_weights[route_id], 0.0)
        grad_rows = (stream_grad[token_id].astype(jnp.float32) * route_scale[:, None]).astype(jnp.bfloat16)
        in_rows = jnp.where(slot_used[:, None], expert_inputs[token_id], jnp.zeros((), jnp.bfloat16))
        return expert_backward(in_rows, grad_rows, gate_weight, up_weight, down_weight)
    grad_gate_proj, grad_up_proj, grad_down_proj, input_grads = lax.map(expert_pass, (slot_table.reshape(EXPERTS, expert_slots), gate_proj, up_proj, down_proj))
    per_route = input_grads.reshape(EXPERTS * expert_slots, D)[slot_index].reshape(TOKENS, TOPK, D)
    stream_total = (stream_grad.astype(jnp.float32) + lax.optimization_barrier(jnp.sum(per_route, axis=1))).astype(jnp.bfloat16)
    across = (((0,), (0,)), ((), ()))
    grad_out_proj = lax.dot_general(stream_total, gated_out, across, preferred_element_type=jnp.float32)
    gated_grad = jnp.dot(stream_total, out_proj, preferred_element_type=jnp.float32).reshape(TOKENS, GROUPS, per_group, HEAD_DIM)
    grad_gate = (gated_grad * mixer_out * gate_sigmoid * (1.0 + gate_in * (1.0 - gate_sigmoid))).reshape(TOKENS, DI).astype(jnp.bfloat16)
    mixer_grad = gated_grad * gate_silu
    grad_vals, grad_in, grad_out, grad_step = back_mixer(mixer_grad)
    return (grad_gate_proj, grad_up_proj, grad_down_proj, grad_out_proj, grad_vals.reshape(TOKENS, DI).astype(jnp.bfloat16), grad_gate, grad_in.reshape(TOKENS, GROUPS * NSTATE).astype(jnp.bfloat16), grad_out.reshape(TOKENS, GROUPS * NSTATE).astype(jnp.bfloat16), grad_step.reshape(TOKENS, HEADS))
```

```python
import functools

import jax
import jax.numpy as jnp
from jax import lax
from jax.experimental import pallas as pl
from jax.experimental.pallas import tpu as pltpu
from jax.sharding import PartitionSpec as P

NSTATE = 128
CLAMP_LIMIT = 7.0
SIGMOID_SCALE = 1.702
HIGHEST = lax.Precision.HIGHEST
F32 = jnp.float32
BF16 = jnp.bfloat16
NN = (((1,), (0,)), ((), ()))
NT = (((1,), (1,)), ((), ()))
TN = (((0,), (0,)), ((), ()))


def mm(a, b, dims=NN):
    return lax.dot_general(a, b, dims, preferred_element_type=F32)


def mm_exact(a, b, dims=NN):
    return lax.dot_general(a, b, dims, precision=HIGHEST, preferred_element_type=F32)


def grid_of(rows, cols):
    return (
        lax.broadcasted_iota(jnp.int32, (rows, cols), 0),
        lax.broadcasted_iota(jnp.int32, (rows, cols), 1),
    )


def spread(heads, size):
    at, col = grid_of(heads, heads * size)
    return ((col >= at * size) & (col < (at + 1) * size)).astype(F32)


def fold(heads, size):
    col, at = grid_of(heads * size, heads)
    return ((col >= at * size) & (col < (at + 1) * size)).astype(F32)


def call(kernel, outs, flops, *args, vmem=None):
    bytes_accessed = sum(a.size * a.dtype.itemsize for a in args)
    bytes_accessed += sum(o.size * o.dtype.itemsize for o in outs)
    return pl.pallas_call(
        kernel,
        out_shape=outs,
        in_specs=[pl.BlockSpec(memory_space=pltpu.VMEM)] * len(args),
        out_specs=[pl.BlockSpec(memory_space=pltpu.VMEM)] * len(outs),
        cost_estimate=pl.CostEstimate(
            flops=flops, bytes_accessed=bytes_accessed, transcendentals=0
        ),
        compiler_params=pltpu.CompilerParams(vmem_limit_bytes=vmem or 24 * 2**20),
    )(*args)


def out(shape, dtype):
    return jax.ShapeDtypeStruct(shape, dtype)


def dispatch_kernel(experts, cap, width, routes_ref, weights_ref, x_ref, g_ref, xs_ref, gs_ref, sel_ref):
    tokens, top = routes_ref.shape
    start = pl.multiple_of(lax.axis_index("tp") * width, 128)
    x = x_ref[:, pl.ds(start, width)]
    g = g_ref[:, pl.ds(start, width)].astype(F32)
    _, expert = grid_of(tokens, experts)
    _, slot = grid_of(tokens, experts * cap)
    row, col = grid_of(tokens, tokens)
    hits = [expert == routes_ref[:, k : k + 1] for k in range(top)]
    named = sum(hit.astype(F32) for hit in hits)
    before = mm((row > col).astype(BF16), named.astype(BF16))
    every = jnp.zeros((tokens, experts * cap), F32)
    grads = jnp.zeros((experts * cap, width), F32)
    for k in range(top):
        rank = jnp.sum(jnp.where(hits[k], before, 0.0), axis=1, keepdims=True).astype(jnp.int32)
        chosen = (slot == routes_ref[:, k : k + 1] * cap + rank).astype(F32)
        every = every + chosen
        grads = grads + mm(chosen.astype(BF16), (g * weights_ref[:, k : k + 1]).astype(BF16), TN)
    picked = every.astype(BF16)
    sel_ref[...] = picked
    xs_ref[...] = mm(picked, x, TN).astype(BF16)
    gs_ref[...] = grads.astype(BF16)


def combine_kernel(width, sel_ref, back_ref, g_ref, out_ref):
    start = pl.multiple_of(lax.axis_index("tp") * width, 128)
    g = g_ref[:, pl.ds(start, width)].astype(F32)
    out_ref[...] = (g + mm(sel_ref[...], back_ref[...])).astype(BF16)


def mixing_of(log_ref, logt_ref, h):
    length = log_ref.shape[0]
    row, col = grid_of(length, length)
    gap = log_ref[:, h : h + 1] - logt_ref[h : h + 1, :]
    return jnp.where(row >= col, jnp.exp(jnp.minimum(gap, 0.0)), 0.0)


def local_kernel(groups, v_ref, b_ref, c_ref, steps_ref, log_ref, logt_ref, y_ref, state_ref):
    heads = steps_ref.shape[1]
    per, size = heads // groups, v_ref.shape[1] // heads
    wide = per * size
    length = v_ref.shape[0]
    expand = spread(heads, size)
    to_end = jnp.exp(log_ref[length - 1 :, :] - log_ref[...])
    x = v_ref[...].astype(F32) * mm_exact(steps_ref[...], expand)
    xe = (x * mm_exact(to_end, expand)).astype(BF16)
    x = x.astype(BF16)
    for g in range(groups):
        keys = b_ref[:, g * NSTATE : (g + 1) * NSTATE]
        scores = mm(c_ref[:, g * NSTATE : (g + 1) * NSTATE], keys, NT)
        parts = []
        for r in range(per):
            h = g * per + r
            att = (scores * mixing_of(log_ref, logt_ref, h)).astype(BF16)
            parts.append(mm(att, x[:, h * size : (h + 1) * size]))
        y_ref[:, g * wide : (g + 1) * wide] = jnp.concatenate(parts, axis=1)
        state_ref[g] = mm(xe[:, g * wide : (g + 1) * wide], keys, TN).astype(BF16)


def weighted_state(all_ref, weights_ref, g, r, per, size):
    h = g * per + r
    total = jnp.zeros((size, NSTATE), F32)
    for j in range(all_ref.shape[0]):
        part = all_ref[j, g, r * size : (r + 1) * size, :].astype(F32)
        total = total + weights_ref[j : j + 1, h : h + 1] * part
    return total


def enter_kernel(groups, all_ref, weights_ref, y_ref, gate_ref, c_ref, log_ref, out_ref, gated_ref, state_ref):
    heads = log_ref.shape[1]
    per, size = heads // groups, y_ref.shape[1] // heads
    wide = per * size
    decay = mm_exact(jnp.exp(log_ref[...]), spread(heads, size))
    for g in range(groups):
        state = jnp.concatenate(
            [weighted_state(all_ref, weights_ref, g, r, per, size) for r in range(per)], axis=0
        ).astype(BF16)
        state_ref[g] = state
        at = slice(g * wide, (g + 1) * wide)
        entered = mm(c_ref[:, g * NSTATE : (g + 1) * NSTATE], state, NT) * decay[:, at]
        mixed = y_ref[:, at] + entered
        out_ref[:, at] = mixed
        gate = gate_ref[:, at].astype(F32)
        gated_ref[:, at] = (mixed * gate * jax.nn.sigmoid(gate)).astype(BF16)


def gate_kernel(groups, grad_ref, out_ref, gate_ref, c_ref, log_ref, gate_grad_ref, mixer_ref, state_ref):
    heads = log_ref.shape[1]
    wide = grad_ref.shape[1] // groups
    decay = mm_exact(jnp.exp(log_ref[...]), spread(heads, grad_ref.shape[1] // heads))
    for g in range(groups):
        at = slice(g * wide, (g + 1) * wide)
        gate = gate_ref[:, at].astype(F32)
        sig = jax.nn.sigmoid(gate)
        grad = grad_ref[:, at]
        gate_grad_ref[:, at] = (grad * out_ref[:, at] * sig * (1.0 + gate * (1.0 - sig))).astype(BF16)
        mixer = grad * gate * sig
        mixer_ref[:, at] = mixer
        keys = c_ref[:, g * NSTATE : (g + 1) * NSTATE]
        state_ref[g] = mm((mixer * decay[:, at]).astype(BF16), keys, TN).astype(BF16)


def inner_kernel(
    groups, v_ref, b_ref, c_ref, steps_ref, log_ref, logt_ref, mixer_ref, state_ref,
    out_keys_ref, in_part_ref, x_part_ref, base_ref,
):
    heads = steps_ref.shape[1]
    per, size = heads // groups, v_ref.shape[1] // heads
    wide = per * size
    length = v_ref.shape[0]
    row, col = grid_of(length, length)
    later = (row <= col).astype(BF16)
    expand = spread(heads, size)
    mixer = mixer_ref[...]
    decayed = mixer * mm_exact(jnp.exp(log_ref[...]), expand)
    decayed_low = decayed.astype(BF16)
    mixer = mixer.astype(BF16)
    x = (v_ref[...].astype(F32) * mm_exact(steps_ref[...], expand)).astype(BF16)
    entering = []
    _, head_at = grid_of(length, heads)
    pairs = jnp.zeros((length, heads), F32)
    for g in range(groups):
        at = slice(g * wide, (g + 1) * wide)
        keys_in = b_ref[:, g * NSTATE : (g + 1) * NSTATE]
        keys_out = c_ref[:, g * NSTATE : (g + 1) * NSTATE]
        scores = mm(keys_out, keys_in, NT)
        score_grad = jnp.zeros((length, length), F32)
        parts = []
        for r in range(per):
            h = g * per + r
            here = slice(h * size, (h + 1) * size)
            mixing = mixing_of(log_ref, logt_ref, h)
            att = scores * mixing
            att_grad = mm(mixer[:, here], x[:, here], NT)
            parts.append(mm(att.astype(BF16), mixer[:, here], TN))
            score_grad = score_grad + att_grad * mixing
            after = mm(later, (att_grad * att).astype(BF16))
            crossing = jnp.sum(jnp.where(col < row, after, 0.0), axis=1, keepdims=True)
            pairs = pairs + jnp.where(head_at == h, crossing, 0.0)
        x_part_ref[:, at] = jnp.concatenate(parts, axis=1)
        score_grad = score_grad.astype(BF16)
        state = state_ref[g]
        out_keys_ref[:, g * NSTATE : (g + 1) * NSTATE] = (
            mm(score_grad, keys_in) + mm(decayed_low[:, at], state)
        ).astype(BF16)
        in_part_ref[:, g * NSTATE : (g + 1) * NSTATE] = mm(score_grad, keys_out, TN)
        entering.append(decayed[:, at] * mm(keys_out, state, NT))
    entering = jnp.concatenate(entering, axis=1)
    sums = mm_exact(entering, fold(heads, size))
    base_ref[...] = pairs + mm_exact((row <= col).astype(F32), sums)


def outer_kernel(
    groups, all_ref, weights_ref, state_ref, v_ref, b_ref, steps_ref, log_ref, rates_ref,
    in_part_ref, x_part_ref, base_ref, values_ref, in_keys_ref, steps_grad_ref,
):
    heads = steps_ref.shape[1]
    per, size = heads // groups, v_ref.shape[1] // heads
    wide = per * size
    length = v_ref.shape[0]
    row, col = grid_of(length, length)
    expand = spread(heads, size)
    last = log_ref[length - 1 :, :]
    steps = mm_exact(steps_ref[...], expand)
    to_end = mm_exact(jnp.exp(last - log_ref[...]), expand)
    values = v_ref[...].astype(F32)
    xe = values * steps * to_end
    xe_low = xe.astype(BF16)
    leaving, direct = [], []
    _, head_at = grid_of(1, heads)
    passing = jnp.zeros((1, heads), F32)
    for g in range(groups):
        at = slice(g * wide, (g + 1) * wide)
        keys_in = b_ref[:, g * NSTATE : (g + 1) * NSTATE]
        tiles = [weighted_state(all_ref, weights_ref, g, r, per, size) for r in range(per)]
        for r in range(per):
            before = state_ref[g, r * size : (r + 1) * size, :].astype(F32)
            both = jnp.sum(jnp.sum(tiles[r] * before, axis=0, keepdims=True), axis=1, keepdims=True)
            passing = passing + jnp.where(head_at == g * per + r, both, 0.0)
        after = jnp.concatenate(tiles, axis=0).astype(BF16)
        reached = mm(keys_in, after, NT)
        x_grad = x_part_ref[:, at] + reached * to_end[:, at]
        values_ref[:, at] = (x_grad * steps[:, at]).astype(BF16)
        in_keys_ref[:, g * NSTATE : (g + 1) * NSTATE] = (
            in_part_ref[:, g * NSTATE : (g + 1) * NSTATE] + mm(xe_low[:, at], after)
        ).astype(BF16)
        leaving.append(reached * xe[:, at])
        direct.append(x_grad * values[:, at])
    gather = fold(heads, size)
    leaving = mm_exact(jnp.concatenate(leaving, axis=1), gather)
    direct = mm_exact(jnp.concatenate(direct, axis=1), gather)
    crossing = base_ref[...] + mm_exact((col < row).astype(F32), leaving) + jnp.exp(last) * passing
    steps_grad_ref[...] = direct - rates_ref[...] * crossing


def side_by_side(stacked):
    return jnp.concatenate([stacked[c] for c in range(stacked.shape[0])], axis=-1)


def body(
    mix_values,
    mix_gate,
    input_keys,
    output_keys,
    step_sizes,
    decay_rates,
    out_proj,
    expert_inputs,
    stream_grad,
    routes,
    route_weights,
    gate_proj,
    up_proj,
    down_proj,
):
    tok_rows = mix_values.shape[0]
    model_width = stream_grad.shape[1]
    top = routes.shape[1]
    sp_devices = lax.axis_size("sp")
    tp_devices = lax.axis_size("tp")
    experts = gate_proj.shape[0] * sp_devices
    cap = 3 * tok_rows * top // (2 * experts)
    slots = experts * cap
    heads = step_sizes.shape[1]
    groups = input_keys.shape[1] // NSTATE
    inner = mix_values.shape[1]
    size = inner // heads
    wide = inner // groups
    width = model_width // tp_devices
    state_shape = (groups, wide, NSTATE)
    pair_flops = 2 * tok_rows * tok_rows * inner

    send_rows, send_grad, chosen = call(
        functools.partial(dispatch_kernel, experts, cap, width),
        [out((slots, width), BF16), out((slots, width), BF16), out((tok_rows, slots), BF16)],
        6 * tok_rows * slots * width,
        routes, route_weights, expert_inputs, stream_grad,
    )

    def to_experts(rows):
        got = lax.all_to_all(
            rows.reshape(experts, cap, width), "sp", split_axis=0, concat_axis=0, tiled=True
        )
        return lax.all_gather(got.reshape(slots, width), "tp", axis=0)

    in_rows = side_by_side(to_experts(send_rows))
    grad_rows = side_by_side(to_experts(send_grad))

    row, col = grid_of(tok_rows, tok_rows)
    rates = decay_rates.reshape(1, heads)
    drop = -step_sizes * rates
    log_decay = mm_exact((row >= col).astype(F32), drop)
    log_decay_t = log_decay.T
    y_local, own_state = call(
        functools.partial(local_kernel, groups),
        [out((tok_rows, inner), F32), out(state_shape, BF16)],
        3 * pair_flops,
        mix_values, input_keys, output_keys, step_sizes, log_decay, log_decay_t,
    )
    spans = lax.all_gather(log_decay[tok_rows - 1], "sp", axis=0)
    here = lax.axis_index("sp")
    order = jnp.arange(sp_devices)
    one, two = order[:, None], order[None, :]
    forward = mm_exact(((two > one) & (two < here)).astype(F32), spans)
    forward = jnp.where(one < here, jnp.exp(forward), 0.0)
    backward = mm_exact(((two < one) & (two > here)).astype(F32), spans)
    backward = jnp.where(one > here, jnp.exp(backward), 0.0)
    all_states = lax.all_gather(own_state, "sp", axis=0)
    mixer_out, gated_out, state_in = call(
        functools.partial(enter_kernel, groups),
        [out((tok_rows, inner), F32), out((tok_rows, inner), BF16), out(state_shape, BF16)],
        2 * pair_flops,
        all_states, forward, y_local, mix_gate, output_keys, log_decay,
    )
    full_proj = lax.all_gather(out_proj, "sp", axis=0, tiled=True)
    all_gated = lax.all_gather(gated_out, "sp", axis=0, tiled=True)

    gate_weight = gate_proj.reshape(-1, model_width)
    up_weight = up_proj.reshape(-1, model_width)
    down_weight = down_proj.reshape(-1, model_width)
    gate_pre = mm(in_rows, gate_weight, NT)
    up_pre = mm(in_rows, up_weight, NT)
    gate_clamped = jnp.minimum(gate_pre, CLAMP_LIMIT)
    up_clamped = jnp.clip(up_pre, -CLAMP_LIMIT, CLAMP_LIMIT)
    gate_sigmoid = jax.nn.sigmoid(SIGMOID_SCALE * gate_clamped)
    activation = ((up_clamped + 1.0) * gate_clamped * gate_sigmoid).astype(BF16)
    act_grad = mm(grad_rows, down_weight, NT)
    gate_grad = jnp.where(
        gate_pre < CLAMP_LIMIT,
        act_grad
        * (up_clamped + 1.0)
        * gate_sigmoid
        * (1.0 + SIGMOID_SCALE * gate_clamped * (1.0 - gate_sigmoid)),
        0.0,
    ).astype(BF16)
    up_grad = jnp.where(
        jnp.abs(up_pre) < CLAMP_LIMIT, act_grad * gate_clamped * gate_sigmoid, 0.0
    ).astype(BF16)
    back = (mm(gate_grad, gate_weight) + mm(up_grad, up_weight)).astype(BF16)
    grad_down_proj = mm(activation, grad_rows, TN).astype(BF16).reshape(down_proj.shape)
    grad_gate_proj = mm(gate_grad, in_rows, TN).astype(BF16).reshape(gate_proj.shape)
    grad_up_proj = mm(up_grad, in_rows, TN).astype(BF16).reshape(up_proj.shape)

    reduced = lax.psum_scatter(back, "tp", scatter_dimension=1, tiled=True)
    returned = lax.all_to_all(
        reduced.reshape(experts, cap, width), "sp", split_axis=0, concat_axis=0, tiled=True
    ).reshape(slots, width)
    stream_part = call(
        functools.partial(combine_kernel, width),
        [out((tok_rows, width), BF16)],
        2 * tok_rows * slots * width,
        chosen, returned, stream_grad,
    )[0]
    stream_total = lax.all_gather(stream_part, "tp", axis=1, tiled=True)

    gated_grad = mm(stream_total, full_proj)
    grad_gate, mixer_grad, own_grad = call(
        functools.partial(gate_kernel, groups),
        [out((tok_rows, inner), BF16), out((tok_rows, inner), F32), out(state_shape, BF16)],
        pair_flops,
        gated_grad, mixer_out, mix_gate, output_keys, log_decay,
    )
    all_grads = lax.all_gather(own_grad, "sp", axis=0)
    share = model_width // sp_devices
    all_stream = lax.all_to_all(
        stream_total, "sp", split_axis=1, concat_axis=0, tiled=True
    ).reshape(sp_devices * tok_rows, share)
    grad_out_proj = mm(all_stream, all_gated, TN)
    grad_output_keys, in_part, x_part, base = call(
        functools.partial(inner_kernel, groups),
        [
            out(output_keys.shape, BF16),
            out(input_keys.shape, F32),
            out((tok_rows, inner), F32),
            out((tok_rows, heads), F32),
        ],
        6 * pair_flops,
        mix_values, input_keys, output_keys, step_sizes, log_decay, log_decay_t, mixer_grad, state_in,
    )
    grad_values, grad_input_keys, grad_steps = call(
        functools.partial(outer_kernel, groups),
        [
            out((tok_rows, inner), BF16),
            out(input_keys.shape, BF16),
            out((tok_rows, heads), F32),
        ],
        3 * pair_flops,
        all_grads, backward, state_in, mix_values, input_keys, step_sizes, log_decay, rates,
        in_part, x_part, base,
    )
    return (
        grad_gate_proj,
        grad_up_proj,
        grad_down_proj,
        grad_out_proj,
        grad_values,
        grad_gate,
        grad_input_keys,
        grad_output_keys,
        grad_steps,
    )


def solution(mesh):
    return jax.shard_map(
        body,
        mesh=mesh,
        in_specs=(
            P("sp", "tp"),
            P("sp", "tp"),
            P("sp", "tp"),
            P("sp", "tp"),
            P("sp", "tp"),
            P("tp"),
            P("sp", "tp"),
            P("sp", None),
            P("sp", None),
            P("sp", None),
            P("sp", None),
            P("sp", "tp", None),
            P("sp", "tp", None),
            P("sp", "tp", None),
        ),
        out_specs=(
            P("sp", "tp", None),
            P("sp", "tp", None),
            P("sp", "tp", None),
            P("sp", "tp"),
            P("sp", "tp"),
            P("sp", "tp"),
            P("sp", "tp"),
            P("sp", "tp"),
            P("sp", "tp"),
        ),
        check_vma=False,
    )
```

```python
import functools

import jax
import jax.numpy as jnp
from jax import lax
from jax.experimental import pallas as pl
from jax.experimental.pallas import tpu as pltpu
from jax.sharding import PartitionSpec as P

NSTATE = 128
TAIL = 16
TERMS = 3
CLAMP_LIMIT = 7.0
SIGMOID_SCALE = 1.702
HIGHEST = lax.Precision.HIGHEST
F32 = jnp.float32
BF16 = jnp.bfloat16
NN = (((1,), (0,)), ((), ()))
NT = (((1,), (1,)), ((), ()))
TN = (((0,), (0,)), ((), ()))


def mm(a, b, dims=NN):
    return lax.dot_general(a, b, dims, preferred_element_type=F32)


def mm_exact(a, b, dims=NN):
    return lax.dot_general(a, b, dims, precision=HIGHEST, preferred_element_type=F32)


def grid_of(rows, cols):
    return (
        lax.broadcasted_iota(jnp.int32, (rows, cols), 0),
        lax.broadcasted_iota(jnp.int32, (rows, cols), 1),
    )


def spread(heads, size):
    at, col = grid_of(heads, heads * size)
    return ((col >= at * size) & (col < (at + 1) * size)).astype(F32)


def fold(heads, size):
    col, at = grid_of(heads * size, heads)
    return ((col >= at * size) & (col < (at + 1) * size)).astype(F32)


def call(kernel, outs, flops, *args, vmem=None):
    bytes_accessed = sum(a.size * a.dtype.itemsize for a in args)
    bytes_accessed += sum(o.size * o.dtype.itemsize for o in outs)
    return pl.pallas_call(
        kernel,
        out_shape=outs,
        in_specs=[pl.BlockSpec(memory_space=pltpu.VMEM)] * len(args),
        out_specs=[pl.BlockSpec(memory_space=pltpu.VMEM)] * len(outs),
        cost_estimate=pl.CostEstimate(
            flops=flops, bytes_accessed=bytes_accessed, transcendentals=0
        ),
        compiler_params=pltpu.CompilerParams(vmem_limit_bytes=vmem or 24 * 2**20),
    )(*args)


def out(shape, dtype):
    return jax.ShapeDtypeStruct(shape, dtype)


def dispatch_kernel(experts, cap, width, routes_ref, weights_ref, x_ref, g_ref, xs_ref, gs_ref, sel_ref):
    tokens, top = routes_ref.shape
    start = pl.multiple_of(lax.axis_index("tp") * width, 128)
    x = x_ref[:, pl.ds(start, width)]
    g = g_ref[:, pl.ds(start, width)].astype(F32)
    _, expert = grid_of(tokens, experts)
    _, slot = grid_of(tokens, experts * cap)
    row, col = grid_of(tokens, tokens)
    hits = [expert == routes_ref[:, k : k + 1] for k in range(top)]
    named = sum(hit.astype(F32) for hit in hits)
    before = mm((row > col).astype(BF16), named.astype(BF16))
    every = jnp.zeros((tokens, experts * cap), F32)
    grads = jnp.zeros((experts * cap, width), F32)
    for k in range(top):
        rank = jnp.sum(jnp.where(hits[k], before, 0.0), axis=1, keepdims=True).astype(jnp.int32)
        chosen = (slot == routes_ref[:, k : k + 1] * cap + rank).astype(F32)
        every = every + chosen
        grads = grads + mm(chosen.astype(BF16), (g * weights_ref[:, k : k + 1]).astype(BF16), TN)
    picked = every.astype(BF16)
    sel_ref[...] = picked
    xs_ref[...] = mm(picked, x, TN).astype(BF16)
    gs_ref[...] = grads.astype(BF16)


def combine_kernel(width, sel_ref, back_ref, g_ref, out_ref):
    start = pl.multiple_of(lax.axis_index("tp") * width, 128)
    g = g_ref[:, pl.ds(start, width)].astype(F32)
    out_ref[...] = (g + mm(sel_ref[...], back_ref[...])).astype(BF16)


def mixing_of(log_ref, logt_ref, h):
    length = log_ref.shape[0]
    row, col = grid_of(length, length)
    gap = log_ref[:, h : h + 1] - logt_ref[h : h + 1, :]
    return jnp.where(row >= col, jnp.exp(jnp.minimum(gap, 0.0)), 0.0)


def local_kernel(groups, v_ref, b_ref, c_ref, steps_ref, log_ref, logt_ref, y_ref, state_ref):
    heads = steps_ref.shape[1]
    per, size = heads // groups, v_ref.shape[1] // heads
    wide = per * size
    length = v_ref.shape[0]
    expand = spread(heads, size)
    to_end = jnp.exp(log_ref[length - 1 :, :] - log_ref[...])
    x = v_ref[...].astype(F32) * mm_exact(steps_ref[...], expand)
    xe = (x * mm_exact(to_end, expand)).astype(BF16)
    x = x.astype(BF16)
    for g in range(groups):
        keys = b_ref[:, g * NSTATE : (g + 1) * NSTATE]
        scores = mm(c_ref[:, g * NSTATE : (g + 1) * NSTATE], keys, NT)
        parts = []
        for r in range(per):
            h = g * per + r
            att = (scores * mixing_of(log_ref, logt_ref, h)).astype(BF16)
            parts.append(mm(att, x[:, h * size : (h + 1) * size]))
        y_ref[:, g * wide : (g + 1) * wide] = jnp.concatenate(parts, axis=1)
        state_ref[g * wide : (g + 1) * wide, :] = mm(
            xe[:, g * wide : (g + 1) * wide], keys, TN
        ).astype(BF16)
    at, lane = grid_of(heads, NSTATE)
    rest = mm_exact(log_ref[length - 1 :, :], (at == lane).astype(F32))
    row, _ = grid_of(TAIL, NSTATE)
    tail = jnp.zeros((TAIL, NSTATE), F32)
    for k in range(TERMS):
        term = rest.astype(BF16).astype(F32)
        tail = jnp.where(row == k, term, tail)
        rest = rest - term
    state_ref[groups * wide :, :] = tail.astype(BF16)


def weighted_state(all_ref, weights_ref, g, r, per, size):
    h = g * per + r
    total = jnp.zeros((size, NSTATE), F32)
    for j in range(all_ref.shape[0]):
        part = all_ref[j, h * size : (h + 1) * size, :].astype(F32)
        total = total + weights_ref[j : j + 1, h : h + 1] * part
    return total


def enter_kernel(groups, all_ref, weights_ref, y_ref, gate_ref, c_ref, log_ref, out_ref, gated_ref, state_ref):
    heads = log_ref.shape[1]
    per, size = heads // groups, y_ref.shape[1] // heads
    wide = per * size
    decay = mm_exact(jnp.exp(log_ref[...]), spread(heads, size))
    for g in range(groups):
        state = jnp.concatenate(
            [weighted_state(all_ref, weights_ref, g, r, per, size) for r in range(per)], axis=0
        ).astype(BF16)
        state_ref[g] = state
        at = slice(g * wide, (g + 1) * wide)
        entered = mm(c_ref[:, g * NSTATE : (g + 1) * NSTATE], state, NT) * decay[:, at]
        mixed = y_ref[:, at] + entered
        out_ref[:, at] = mixed
        gate = gate_ref[:, at].astype(F32)
        gated_ref[:, at] = (mixed * gate * jax.nn.sigmoid(gate)).astype(BF16)


def gate_kernel(groups, grad_ref, out_ref, gate_ref, c_ref, log_ref, gate_grad_ref, mixer_ref, state_ref):
    heads = log_ref.shape[1]
    wide = grad_ref.shape[1] // groups
    decay = mm_exact(jnp.exp(log_ref[...]), spread(heads, grad_ref.shape[1] // heads))
    for g in range(groups):
        at = slice(g * wide, (g + 1) * wide)
        gate = gate_ref[:, at].astype(F32)
        sig = jax.nn.sigmoid(gate)
        grad = grad_ref[:, at]
        gate_grad_ref[:, at] = (grad * out_ref[:, at] * sig * (1.0 + gate * (1.0 - sig))).astype(BF16)
        mixer = grad * gate * sig
        mixer_ref[:, at] = mixer
        keys = c_ref[:, g * NSTATE : (g + 1) * NSTATE]
        state_ref[at, :] = mm((mixer * decay[:, at]).astype(BF16), keys, TN).astype(BF16)


def inner_kernel(
    groups, v_ref, b_ref, c_ref, steps_ref, log_ref, logt_ref, mixer_ref, state_ref,
    out_keys_ref, in_part_ref, x_part_ref, base_ref,
):
    heads = steps_ref.shape[1]
    per, size = heads // groups, v_ref.shape[1] // heads
    wide = per * size
    length = v_ref.shape[0]
    row, col = grid_of(length, length)
    later = (row <= col).astype(BF16)
    expand = spread(heads, size)
    mixer = mixer_ref[...]
    decayed = mixer * mm_exact(jnp.exp(log_ref[...]), expand)
    decayed_low = decayed.astype(BF16)
    mixer = mixer.astype(BF16)
    x = (v_ref[...].astype(F32) * mm_exact(steps_ref[...], expand)).astype(BF16)
    entering = []
    _, head_at = grid_of(length, heads)
    pairs = jnp.zeros((length, heads), F32)
    for g in range(groups):
        at = slice(g * wide, (g + 1) * wide)
        keys_in = b_ref[:, g * NSTATE : (g + 1) * NSTATE]
        keys_out = c_ref[:, g * NSTATE : (g + 1) * NSTATE]
        scores = mm(keys_out, keys_in, NT)
        score_grad = jnp.zeros((length, length), F32)
        parts = []
        for r in range(per):
            h = g * per + r
            here = slice(h * size, (h + 1) * size)
            mixing = mixing_of(log_ref, logt_ref, h)
            att = scores * mixing
            att_grad = mm(mixer[:, here], x[:, here], NT)
            parts.append(mm(att.astype(BF16), mixer[:, here], TN))
            score_grad = score_grad + att_grad * mixing
            after = mm(later, (att_grad * att).astype(BF16))
            crossing = jnp.sum(jnp.where(col < row, after, 0.0), axis=1, keepdims=True)
            pairs = pairs + jnp.where(head_at == h, crossing, 0.0)
        x_part_ref[:, at] = jnp.concatenate(parts, axis=1)
        score_grad = score_grad.astype(BF16)
        state = state_ref[g]
        out_keys_ref[:, g * NSTATE : (g + 1) * NSTATE] = (
            mm(score_grad, keys_in) + mm(decayed_low[:, at], state)
        ).astype(BF16)
        in_part_ref[:, g * NSTATE : (g + 1) * NSTATE] = mm(score_grad, keys_out, TN)
        entering.append(decayed[:, at] * mm(keys_out, state, NT))
    entering = jnp.concatenate(entering, axis=1)
    sums = mm_exact(entering, fold(heads, size))
    base_ref[...] = pairs + mm_exact((row <= col).astype(F32), sums)


def outer_kernel(
    groups, all_ref, weights_ref, state_ref, v_ref, b_ref, steps_ref, log_ref, rates_ref,
    in_part_ref, x_part_ref, base_ref, values_ref, in_keys_ref, steps_grad_ref,
):
    heads = steps_ref.shape[1]
    per, size = heads // groups, v_ref.shape[1] // heads
    wide = per * size
    length = v_ref.shape[0]
    row, col = grid_of(length, length)
    expand = spread(heads, size)
    last = log_ref[length - 1 :, :]
    steps = mm_exact(steps_ref[...], expand)
    to_end = mm_exact(jnp.exp(last - log_ref[...]), expand)
    values = v_ref[...].astype(F32)
    xe = values * steps * to_end
    xe_low = xe.astype(BF16)
    leaving, direct = [], []
    _, head_at = grid_of(1, heads)
    passing = jnp.zeros((1, heads), F32)
    for g in range(groups):
        at = slice(g * wide, (g + 1) * wide)
        keys_in = b_ref[:, g * NSTATE : (g + 1) * NSTATE]
        tiles = [weighted_state(all_ref, weights_ref, g, r, per, size) for r in range(per)]
        for r in range(per):
            before = state_ref[g, r * size : (r + 1) * size, :].astype(F32)
            both = jnp.sum(jnp.sum(tiles[r] * before, axis=0, keepdims=True), axis=1, keepdims=True)
            passing = passing + jnp.where(head_at == g * per + r, both, 0.0)
        after = jnp.concatenate(tiles, axis=0).astype(BF16)
        reached = mm(keys_in, after, NT)
        x_grad = x_part_ref[:, at] + reached * to_end[:, at]
        values_ref[:, at] = (x_grad * steps[:, at]).astype(BF16)
        in_keys_ref[:, g * NSTATE : (g + 1) * NSTATE] = (
            in_part_ref[:, g * NSTATE : (g + 1) * NSTATE] + mm(xe_low[:, at], after)
        ).astype(BF16)
        leaving.append(reached * xe[:, at])
        direct.append(x_grad * values[:, at])
    gather = fold(heads, size)
    leaving = mm_exact(jnp.concatenate(leaving, axis=1), gather)
    direct = mm_exact(jnp.concatenate(direct, axis=1), gather)
    crossing = base_ref[...] + mm_exact((col < row).astype(F32), leaving) + jnp.exp(last) * passing
    steps_grad_ref[...] = direct - rates_ref[...] * crossing


def side_by_side(stacked):
    return jnp.concatenate([stacked[c] for c in range(stacked.shape[0])], axis=-1)


def body(
    mix_values,
    mix_gate,
    input_keys,
    output_keys,
    step_sizes,
    decay_rates,
    out_proj,
    expert_inputs,
    stream_grad,
    routes,
    route_weights,
    gate_proj,
    up_proj,
    down_proj,
):
    tok_rows = mix_values.shape[0]
    model_width = stream_grad.shape[1]
    top = routes.shape[1]
    sp_devices = lax.axis_size("sp")
    tp_devices = lax.axis_size("tp")
    experts = gate_proj.shape[0] * sp_devices
    cap = 3 * tok_rows * top // (2 * experts)
    slots = experts * cap
    heads = step_sizes.shape[1]
    groups = input_keys.shape[1] // NSTATE
    inner = mix_values.shape[1]
    size = inner // heads
    wide = inner // groups
    width = model_width // tp_devices
    state_shape = (groups, wide, NSTATE)
    pair_flops = 2 * tok_rows * tok_rows * inner

    row, col = grid_of(tok_rows, tok_rows)
    rates = decay_rates.reshape(1, heads)
    drop = -step_sizes * rates
    log_decay = mm_exact((row >= col).astype(F32), drop)
    log_decay_t = log_decay.T
    y_local, own_state = call(
        functools.partial(local_kernel, groups),
        [out((tok_rows, inner), F32), out((inner + TAIL, NSTATE), BF16)],
        3 * pair_flops,
        mix_values, input_keys, output_keys, step_sizes, log_decay, log_decay_t,
    )
    all_states = lax.all_gather(own_state, "sp", axis=0)

    send_rows, send_grad, chosen = call(
        functools.partial(dispatch_kernel, experts, cap, width),
        [out((slots, width), BF16), out((slots, width), BF16), out((tok_rows, slots), BF16)],
        6 * tok_rows * slots * width,
        routes, route_weights, expert_inputs, stream_grad,
    )

    def over_sp(rows):
        return lax.all_to_all(
            rows.reshape(experts, cap, width), "sp", split_axis=0, concat_axis=0, tiled=True
        ).reshape(slots, width)

    def over_tp(part):
        copies = jnp.broadcast_to(part[None], (tp_devices,) + part.shape)
        return lax.all_to_all(copies, "tp", split_axis=0, concat_axis=0, tiled=True)

    got_rows = over_sp(send_rows)
    got_grad, all_states = lax.optimization_barrier((over_sp(send_grad), all_states))
    in_rows = side_by_side(over_tp(got_rows))
    grad_rows = side_by_side(over_tp(got_grad))

    spans = jnp.sum(all_states[:, inner : inner + TERMS, :heads].astype(F32), axis=1)
    here = lax.axis_index("sp")
    order = jnp.arange(sp_devices)
    one, two = order[:, None], order[None, :]
    forward = mm_exact(((two > one) & (two < here)).astype(F32), spans)
    forward = jnp.where(one < here, jnp.exp(forward), 0.0)
    backward = mm_exact(((two < one) & (two > here)).astype(F32), spans)
    backward = jnp.where(one > here, jnp.exp(backward), 0.0)
    mixer_out, gated_out, state_in = call(
        functools.partial(enter_kernel, groups),
        [out((tok_rows, inner), F32), out((tok_rows, inner), BF16), out(state_shape, BF16)],
        2 * pair_flops,
        all_states, forward, y_local, mix_gate, output_keys, log_decay,
    )
    gate_weight = gate_proj.reshape(-1, model_width)
    up_weight = up_proj.reshape(-1, model_width)
    down_weight = down_proj.reshape(-1, model_width)
    gate_pre = mm(in_rows, gate_weight, NT)
    up_pre = mm(in_rows, up_weight, NT)
    gate_clamped = jnp.minimum(gate_pre, CLAMP_LIMIT)
    up_clamped = jnp.clip(up_pre, -CLAMP_LIMIT, CLAMP_LIMIT)
    gate_sigmoid = jax.nn.sigmoid(SIGMOID_SCALE * gate_clamped)
    activation = ((up_clamped + 1.0) * gate_clamped * gate_sigmoid).astype(BF16)
    act_grad = mm(grad_rows, down_weight, NT)
    gate_grad = jnp.where(
        gate_pre < CLAMP_LIMIT,
        act_grad
        * (up_clamped + 1.0)
        * gate_sigmoid
        * (1.0 + SIGMOID_SCALE * gate_clamped * (1.0 - gate_sigmoid)),
        0.0,
    ).astype(BF16)
    up_grad = jnp.where(
        jnp.abs(up_pre) < CLAMP_LIMIT, act_grad * gate_clamped * gate_sigmoid, 0.0
    ).astype(BF16)
    back = (mm(gate_grad, gate_weight) + mm(up_grad, up_weight)).astype(BF16)
    grad_down_proj = mm(activation, grad_rows, TN).astype(BF16).reshape(down_proj.shape)
    grad_gate_proj = mm(gate_grad, in_rows, TN).astype(BF16).reshape(gate_proj.shape)
    grad_up_proj = mm(up_grad, in_rows, TN).astype(BF16).reshape(up_proj.shape)

    full_proj = lax.all_gather(out_proj, "sp", axis=0, tiled=True)
    back, full_proj, gated_out = lax.optimization_barrier((back, full_proj, gated_out))
    all_gated = lax.all_gather(gated_out, "sp", axis=0, tiled=True)
    shares = jnp.stack([back[:, c * width : (c + 1) * width] for c in range(tp_devices)])
    shares = lax.all_to_all(shares, "tp", split_axis=0, concat_axis=0, tiled=True)
    reduced = jnp.sum(shares.astype(F32), axis=0).astype(BF16)
    returned = lax.all_to_all(
        reduced.reshape(experts, cap, width), "sp", split_axis=0, concat_axis=0, tiled=True
    ).reshape(slots, width)
    stream_part = call(
        functools.partial(combine_kernel, width),
        [out((tok_rows, width), BF16)],
        2 * tok_rows * slots * width,
        chosen, returned, stream_grad,
    )[0]
    stream_part, all_gated = lax.optimization_barrier((stream_part, all_gated))
    stream_total = lax.all_gather(stream_part, "tp", axis=1, tiled=True)

    gated_grad = mm(stream_total, full_proj)
    grad_gate, mixer_grad, own_grad = call(
        functools.partial(gate_kernel, groups),
        [out((tok_rows, inner), BF16), out((tok_rows, inner), F32), out((inner, NSTATE), BF16)],
        pair_flops,
        gated_grad, mixer_out, mix_gate, output_keys, log_decay,
    )
    all_grads = lax.all_gather(own_grad, "sp", axis=0)
    share = model_width // sp_devices
    all_stream = lax.all_to_all(
        stream_total, "sp", split_axis=1, concat_axis=0, tiled=True
    ).reshape(sp_devices * tok_rows, share)
    grad_out_proj = mm(all_stream, all_gated, TN)
    grad_output_keys, in_part, x_part, base = call(
        functools.partial(inner_kernel, groups),
        [
            out(output_keys.shape, BF16),
            out(input_keys.shape, F32),
            out((tok_rows, inner), F32),
            out((tok_rows, heads), F32),
        ],
        6 * pair_flops,
        mix_values, input_keys, output_keys, step_sizes, log_decay, log_decay_t, mixer_grad, state_in,
    )
    grad_values, grad_input_keys, grad_steps = call(
        functools.partial(outer_kernel, groups),
        [
            out((tok_rows, inner), BF16),
            out(input_keys.shape, BF16),
            out((tok_rows, heads), F32),
        ],
        3 * pair_flops,
        all_grads, backward, state_in, mix_values, input_keys, step_sizes, log_decay, rates,
        in_part, x_part, base,
    )
    return (
        grad_gate_proj,
        grad_up_proj,
        grad_down_proj,
        grad_out_proj,
        grad_values,
        grad_gate,
        grad_input_keys,
        grad_output_keys,
        grad_steps,
    )


def solution(mesh):
    return jax.shard_map(
        body,
        mesh=mesh,
        in_specs=(
            P("sp", "tp"),
            P("sp", "tp"),
            P("sp", "tp"),
            P("sp", "tp"),
            P("sp", "tp"),
            P("tp"),
            P("sp", "tp"),
            P("sp", None),
            P("sp", None),
            P("sp", None),
            P("sp", None),
            P("sp", "tp", None),
            P("sp", "tp", None),
            P("sp", "tp", None),
        ),
        out_specs=(
            P("sp", "tp", None),
            P("sp", "tp", None),
            P("sp", "tp", None),
            P("sp", "tp"),
            P("sp", "tp"),
            P("sp", "tp"),
            P("sp", "tp"),
            P("sp", "tp"),
            P("sp", "tp"),
        ),
        check_vma=False,
    )
```
